32 devices in a mesh: ep: 8 (over z, y), tp: 4 (over x, core).
Axes of the slice: x: 2, y: 2, z: 4, core: 2. Of those that a mesh axis runs over, the one named last changes fastest.
Arguments:
- tokens: bfloat16 [2048, 2048], P('ep', 'tp'), may hold values from -72 to 72
- norm_gain: bfloat16 [2048], P('tp'), may hold values from 0.099609375 to 1.8984375
- expert_ids: int32 [2048, 2], P('ep'), may hold values from 0 to 7, all different within a row; in each aligned block of 256 rows (0 to 255, 256 to 511, ...) at most 128 rows name the same one
- gate_share: float32 [2048, 2], P('ep'), may hold values from 0.1 to 1
- gate_weight: bfloat16 [8, 2048, 4096], P('ep', None, 'tp'), may hold values from -0.125 to 0.125
- up_weight: bfloat16 [8, 2048, 4096], P('ep', None, 'tp'), may hold values from -0.125 to 0.125
- down_weight: bfloat16 [8, 4096, 2048], P('ep', 'tp'), may hold values from -0.09375 to 0.09375
Outputs:
- mixed: bfloat16 [2048, 2048], P('ep', 'tp')
The draws below stay inside these ranges and needn't reach their ends.
Inputs may be any that keep to these rules, and one draw needn't show every extreme that they name: `expert_ids`: each token names two different experts; among the 256 tokens of one index of ep no expert is named more than 128 times, a bound that some block reaches.
All inputs are finite; a program needn't handle non-finite values.
Results may differ from the reference program's by a relative error of at most 0.019.
Values may be sent and summed in bfloat16 or wider, within the bound.
No kernel may reach another device: no remote copies, remote signals or barrier semaphores. Data moves between devices by JAX's collectives and lax.ppermute only.
A program may use at most 64 MiB of HBM per device.

```python
import math
import jax
import jax.numpy as jnp
import numpy as np
from jax import lax

D = 2048
FF = 4096
TOK_DEV = 256
EXPERTS = 8
CAP = 128
TOKENS = 2048
N_EP = 8
N_TP = 4


def draw_tokens(key, part):
    first, second, third = jax.random.split(key, 3)
    scales = jnp.exp(jax.random.uniform(second, (N_TP,), jnp.float32, jnp.log(0.3), jnp.log(3.0)))
    columns = jnp.repeat(scales, D // N_TP)
    base = jnp.clip(jax.random.normal(first, (TOKENS, D), jnp.float32), -6.0, 6.0)
    return (base * columns[None, :]).astype(jnp.bfloat16)


def levels(rng, extent, pieces, smallest, high):
    def one(dim, shards_of):
        draws = jax.random.uniform(jax.random.fold_in(jax.random.fold_in(rng, 6), dim), (shards_of,), jnp.float32, smallest / len(pieces), high / len(pieces))
        return jnp.repeat(jnp.exp(draws), extent[dim] // shards_of).reshape((-1,) + (1,) * (len(extent) - dim - 1))

    factor_of = one(*pieces[0])
    for cut in pieces[1:]:
        factor_of = factor_of * one(*cut)
    return factor_of


def routed_block(own_key, own, number, rows, count, top, most, skew):
    ranking = jax.random.permutation(own_key, count)
    packed, common = portions_of(count, rows * top, most, skew, True), portions_of(count, rows * top, most, skew, False)
    places = jnp.arange(count)

    def named(lengths, turn):
        used = int((lengths > 0).sum())
        fixed = max(1, used // 4)
        passed = fixed + (places - fixed + turn * (used - fixed)) % max(1, count - fixed)
        return jnp.zeros((count,), jnp.int32).at[ranking[jnp.where(places < fixed, places, passed)]].set(jnp.asarray(lengths, jnp.int32))

    lengths = jnp.where(number % 4 == 0, named(packed, number // 4), named(common, number - number // 4 - 1))
    mixed = jax.random.permutation(jax.random.fold_in(own, 3), count)
    source_of, sink = mixed[0:count // 2 * 2:2], mixed[1:count // 2 * 2:2]
    slack = jnp.minimum(lengths[source_of] - 1, most - lengths[sink]) // 2
    slack = jnp.where((source_of == ranking[0]) | (sink == ranking[0]) | (lengths[sink] == 0), 0, jnp.maximum(slack, 0))
    passed = jax.random.randint(jax.random.fold_in(own, 4), (count // 2,), 0, 1 << 20) % (slack + 1)
    lengths = lengths.at[source_of].add(-passed).at[sink].add(passed)
    members = jnp.searchsorted(jnp.cumsum(lengths), jnp.arange(rows * top), side="right").astype(jnp.int32)
    table = members.reshape(top, rows).T
    table = table[jax.random.permutation(jax.random.fold_in(own, 1), rows)]
    turn = jax.random.randint(jax.random.fold_in(own, 2), (rows, 1), 0, top)
    return jnp.take_along_axis(table, (jnp.arange(top)[None, :] + turn) % top, axis=1)


def portions_of(count, total, limit, skew, full):
    loads = [(1 << 20) // math.isqrt(standing ** skew) + 1 for standing in range(1, count + 1)]
    largest = limit if full else min(limit, max(-(-total // count), total * loads[0] // sum(loads)))
    least = 1 if total - largest >= count - 1 else 0
    given, spare = [largest] + [least] * (count - 1), total - largest - least * (count - 1)
    while spare > 0:
        free = [i for i in range(1, count) if given[i] < largest] or [i for i in range(1, count) if given[i] < limit]
        mass, remaining = sum([loads[i] for i in free]), spare
        for i in free:
            addition = min(limit - given[i], max(1, remaining * loads[i] // mass), spare)
            given[i] = given[i] + addition
            spare = spare - addition
    return np.array(given)


def normal_values(own_key, shape, scale, most, shards=(), kind=jnp.bfloat16):
    result = scale * jax.random.normal(own_key, shape, jnp.float32)
    if shards:
        result = result * levels(own_key, shape, shards, -0.22, 0.18)
    return jnp.clip(result, -most, most).astype(kind)


def setup_inputs(seed: int = 0) -> dict:
    arg_keys = jax.random.split(jax.random.key(seed), 8)
    tokens = draw_tokens(jax.random.fold_in(arg_keys[7], 71), 0)
    norm_gain = jnp.clip(1.0 + 0.18 * jax.random.normal(arg_keys[1], (D,), jnp.float32), 0.099609375, 1.8984375).astype(jnp.bfloat16)
    expert_ids_keys = jax.random.split(jax.random.fold_in(arg_keys[2], 1), TOKENS // TOK_DEV)
    expert_ids_turns = jax.random.permutation(jax.random.fold_in(arg_keys[2], 3), TOKENS // TOK_DEV)
    expert_ids = jax.vmap(lambda own, number: routed_block(jax.random.fold_in(arg_keys[2], 2), own, number, TOK_DEV, EXPERTS, 2, CAP, 2))(expert_ids_keys, expert_ids_turns).reshape((TOKENS, 2))
    gate_share = jnp.clip(0.1 + 0.9 * jax.random.uniform(arg_keys[3], (TOKENS, 2), jnp.float32) ** levels(arg_keys[3], (TOKENS, 2), ((0, 8),), -0.2, 0.2), 0.1, 1.0)
    gate_weight = normal_values(arg_keys[4], (EXPERTS, D, FF), D ** -0.5, 0.125, ((0, 8), (2, 4)))
    up_weight = normal_values(arg_keys[5], (EXPERTS, D, FF), D ** -0.5, 0.125, ((0, 8), (2, 4)))
    down_weight = normal_values(arg_keys[6], (EXPERTS, FF, D), FF ** -0.5, 0.09375, ((0, 8), (1, 4)))
    return {"tokens": tokens, "norm_gain": norm_gain, "expert_ids": expert_ids, "gate_share": gate_share, "gate_weight": gate_weight, "up_weight": up_weight, "down_weight": down_weight}


EPS = 1e-06

def reference(tokens, norm_gain, expert_ids, gate_share, gate_weight, up_weight, down_weight):
    xf = tokens.astype(jnp.float32)
    factor = lax.rsqrt(lax.optimization_barrier(jnp.mean(xf * xf, axis=1, keepdims=True)) + EPS)
    normed = (xf * factor * norm_gain.astype(jnp.float32)[None, :]).astype(jnp.bfloat16)
    blocks = expert_ids.reshape(N_EP, TOK_DEV * 2)
    onehot = (blocks[:, :, None] == jnp.arange(EXPERTS, dtype=jnp.int32)[None, None, :]).astype(jnp.int32)
    slots = lax.optimization_barrier(jnp.sum((jnp.cumsum(onehot, axis=1) - onehot) * onehot, axis=2))
    source = jnp.arange(N_EP, dtype=jnp.int32)[:, None]
    position = (source * CAP + slots).reshape(-1).astype(jnp.int32)
    flat_ids = expert_ids.reshape(-1).astype(jnp.int32)
    rows = jnp.repeat(normed, 2, axis=0)
    buffer = jnp.zeros((EXPERTS, N_EP * CAP, D), jnp.bfloat16).at[flat_ids, position].set(rows)
    width = FF // N_TP

    def expert(args):
        buf, w_gate, w_up, w_down = args
        gate = jnp.dot(buf, w_gate, preferred_element_type=jnp.float32)
        upper = jnp.dot(buf, w_up, preferred_element_type=jnp.float32)
        hidden = (jax.nn.silu(gate) * upper).astype(jnp.bfloat16)

        def add_block(index, total):
            piece = lax.dynamic_slice_in_dim(hidden, index * width, width, 1)
            wpiece = lax.dynamic_slice_in_dim(w_down, index * width, width, 0)
            term = jnp.dot(piece, wpiece, preferred_element_type=jnp.float32).astype(jnp.bfloat16)
            return total + lax.optimization_barrier(term).astype(jnp.float32)
        total = lax.fori_loop(0, N_TP, add_block, jnp.zeros((buf.shape[0], D), jnp.float32))
        return total.astype(jnp.bfloat16)
    outputs = lax.map(expert, (buffer, gate_weight, up_weight, down_weight))
    picked = outputs[flat_ids, position].astype(jnp.float32).reshape(TOKENS, 2, D)
    return lax.optimization_barrier(jnp.sum(picked * gate_share[:, :, None], axis=1)).astype(jnp.bfloat16)
```

```python
import functools

import jax
import jax.numpy as jnp
from jax import lax
from jax.experimental import pallas as pl
from jax.experimental.pallas import tpu as pltpu
from jax.sharding import PartitionSpec as P

EPS = 1e-06
MIB = 1024 * 1024
VMEM = pl.BlockSpec(memory_space=pltpu.VMEM)
SMEM = pl.BlockSpec(memory_space=pltpu.SMEM)


def swap(value, axis, bits):
    n = lax.axis_size(axis)
    return lax.ppermute(value, axis, [(i, i ^ bits) for i in range(n)])


def dispatch_kernel(me_ref, ids_ref, tokens_ref, *outs, experts, cap):
    rows = tokens_ref.shape[0]
    expert = lax.broadcasted_iota(jnp.int32, (experts, rows), 0) ^ me_ref[0]
    named = (ids_ref[0:1, :] == expert) | (ids_ref[1:2, :] == expert)
    earlier = lax.broadcasted_iota(jnp.int32, (rows, rows), 0) < lax.broadcasted_iota(jnp.int32, (rows, rows), 1)
    slots = jnp.dot(
        named.astype(jnp.bfloat16), earlier.astype(jnp.bfloat16), preferred_element_type=jnp.float32
    ).astype(jnp.int32)
    slots = jnp.where(named, slots, -1)
    place = lax.broadcasted_iota(jnp.int32, (cap, rows), 0)
    tokens = tokens_ref[...]
    group = experts // len(outs)
    for c, out in enumerate(outs):
        pick = [(place == slots[k : k + 1, :]).astype(jnp.float32) for k in range(c * group, (c + 1) * group)]
        pick = jnp.concatenate(pick, axis=0).astype(jnp.bfloat16)
        out[...] = jnp.dot(pick, tokens, preferred_element_type=jnp.float32).astype(jnp.bfloat16)


def place_kernel(me_ref, ids_ref, out_ref, *, experts, cap):
    rows = ids_ref.shape[0]
    expert = lax.broadcasted_iota(jnp.int32, (rows, experts), 1) ^ me_ref[0]
    first = ids_ref[:, 0:1] == expert
    second = ids_ref[:, 1:2] == expert
    later = lax.broadcasted_iota(jnp.int32, (rows, rows), 0) > lax.broadcasted_iota(jnp.int32, (rows, rows), 1)
    slots = jnp.dot(
        later.astype(jnp.bfloat16), (first | second).astype(jnp.bfloat16), preferred_element_type=jnp.float32
    ).astype(jnp.int32)
    target = slots + cap * lax.broadcasted_iota(jnp.int32, (rows, experts), 1)
    for j, chosen in enumerate((first, second)):
        out_ref[:, j : j + 1] = jnp.sum(jnp.where(chosen, target, 0), axis=1, keepdims=True)


def combine_kernel(target_ref, share_ref, *refs):
    blocks, out, table = refs[:-2], refs[-2], refs[-1]
    cap = blocks[0].shape[0]
    for k, block in enumerate(blocks):
        table[k * cap : (k + 1) * cap, :] = block[...]
    rows = out.shape[0]
    total = jnp.zeros(out.shape, jnp.float32)
    slot = lax.broadcasted_iota(jnp.int32, (rows, table.shape[0]), 1)
    for j in range(2):
        pick = (slot == target_ref[:, j : j + 1]).astype(jnp.float32).astype(jnp.bfloat16)
        found = jnp.dot(pick, table[...], preferred_element_type=jnp.float32)
        total = total + found * share_ref[:, j : j + 1]
    out[...] = total.astype(jnp.bfloat16)


def ffn_kernel(me_ref, *refs, n_tp, block):
    pieces = refs[:n_tp]
    gain_ref, gate_ref, up_ref, down_ref, keep_ref, give_ref, normed_ref, hidden_ref = refs[n_tp:]
    me = me_ref[0]
    rows, width = pieces[0].shape
    squares = jnp.zeros((rows, 1), jnp.float32)
    for piece in pieces:
        values = piece[...].astype(jnp.float32)
        squares = squares + jnp.sum(values * values, axis=1, keepdims=True)
    factor = lax.rsqrt(squares / gate_ref.shape[0] + EPS)
    for j, piece in enumerate(pieces):
        at = pl.ds(pl.multiple_of((me ^ j) * width, width), width)
        scaled = piece[...].astype(jnp.float32) * factor * gain_ref[:, at].astype(jnp.float32)
        normed_ref[:, at] = scaled.astype(jnp.bfloat16)
    normed = normed_ref[...]
    for o in range(0, gate_ref.shape[1], block):
        gate = jnp.dot(normed, gate_ref[:, o : o + block], preferred_element_type=jnp.float32)
        upper = jnp.dot(normed, up_ref[:, o : o + block], preferred_element_type=jnp.float32)
        hidden_ref[:, o : o + block] = (gate / (1.0 + jnp.exp(-gate)) * upper).astype(jnp.bfloat16)
    hidden = hidden_ref[...]
    for j in range(n_tp):
        at = pl.ds(pl.multiple_of((me ^ j) * width, width), width)
        term = jnp.dot(hidden, down_ref[:, at], preferred_element_type=jnp.float32).astype(jnp.bfloat16)
        ref = (keep_ref, give_ref)[j & 1]
        ref[(j >> 1) * rows : ((j >> 1) + 1) * rows, :] = term


def ffn(me, pieces, gain, gate_weight, up_weight, down_weight):
    rows, width = pieces[0].shape
    n_tp = len(pieces)
    d, f = gate_weight.shape
    half = jax.ShapeDtypeStruct((n_tp // 2 * rows, width), jnp.bfloat16)
    return pl.pallas_call(
        functools.partial(ffn_kernel, n_tp=n_tp, block=min(f, 512)),
        out_shape=(half, half),
        in_specs=[SMEM] + [VMEM] * (n_tp + 4),
        out_specs=(VMEM, VMEM),
        scratch_shapes=[pltpu.VMEM((rows, d), jnp.bfloat16), pltpu.VMEM((rows, f), jnp.bfloat16)],
        compiler_params=pltpu.CompilerParams(vmem_limit_bytes=40 * MIB),
        name="ffn",
    )(me, *pieces, gain, gate_weight, up_weight, down_weight)


def shards(tokens, norm_gain, expert_ids, gate_share, gate_weight, up_weight, down_weight):
    n_ep, n_tp = lax.axis_size("ep"), lax.axis_size("tp")
    rows, width = tokens.shape
    experts = n_ep
    cap = 4 * rows // experts
    ep = lax.axis_index("ep").reshape(1).astype(jnp.int32)
    tp = lax.axis_index("tp").reshape(1).astype(jnp.int32)
    bits = [1 << b for b in range(n_tp.bit_length() - 1)]

    sends = pl.pallas_call(
        functools.partial(dispatch_kernel, experts=experts, cap=cap),
        out_shape=[jax.ShapeDtypeStruct((cap, width), jnp.bfloat16)] * n_ep,
        in_specs=[SMEM, VMEM, VMEM],
        out_specs=[VMEM] * n_ep,
        compiler_params=pltpu.CompilerParams(vmem_limit_bytes=16 * MIB),
        name="dispatch",
    )(ep, expert_ids.T, tokens)

    gains = [norm_gain.reshape(1, width)]
    for bit in reversed(bits):
        gains = gains + [swap(g, "tp", bit) for g in gains]
    order = [0]
    for bit in reversed(bits):
        order = order + [o ^ bit for o in order]
    gain = jnp.zeros((1, n_tp * width), norm_gain.dtype)
    for o, g in zip(order, gains):
        gain = lax.dynamic_update_slice(gain, g, (0, (tp[0] ^ o) * width))

    arrived = [sends[0]] + [swap(sends[k], "ep", k) for k in range(1, n_ep)]
    group = n_ep // 4
    back = [None] * n_ep
    for c in range(4):
        names = list(range(c * group, (c + 1) * group))
        pieces = {0: jnp.concatenate([arrived[k] for k in names], axis=0)}
        for bit in reversed(bits):
            pieces.update({o ^ bit: swap(p, "tp", bit) for o, p in pieces.items()})
        keep, give = ffn(tp, [pieces[o] for o in range(n_tp)], gain, gate_weight[0], up_weight[0], down_weight[0])
        sums = keep, swap(give, "tp", 1)
        total = (sums[0].astype(jnp.float32) + sums[1].astype(jnp.float32)).astype(jnp.bfloat16)
        size = group * cap
        parts = [total[i * size : (i + 1) * size] for i in range(n_tp // 2)]
        while len(parts) > 1:
            bit = n_tp // len(parts)
            stay, go = parts[0::2], parts[1::2]
            got = [swap(g, "tp", bit) for g in go]
            parts = [
                (s.astype(jnp.float32) + g.astype(jnp.float32)).astype(jnp.bfloat16) for s, g in zip(stay, got)
            ]
        for i, k in enumerate(names):
            piece = parts[0][i * cap : (i + 1) * cap]
            back[k] = swap(piece, "ep", k) if k else piece

    target = pl.pallas_call(
        functools.partial(place_kernel, experts=experts, cap=cap),
        out_shape=jax.ShapeDtypeStruct((rows, 2), jnp.int32),
        in_specs=[SMEM, VMEM],
        out_specs=VMEM,
        compiler_params=pltpu.CompilerParams(vmem_limit_bytes=16 * MIB),
        name="place",
    )(ep, expert_ids)
    return pl.pallas_call(
        combine_kernel,
        out_shape=jax.ShapeDtypeStruct((rows, width), jnp.bfloat16),
        in_specs=[VMEM] * (2 + n_ep),
        out_specs=VMEM,
        scratch_shapes=[pltpu.VMEM((experts * cap, width), jnp.bfloat16)],
        compiler_params=pltpu.CompilerParams(vmem_limit_bytes=16 * MIB),
        name="combine",
    )(target, gate_share, *back)


def solution(mesh):
    in_specs = (
        P("ep", "tp"),
        P("tp"),
        P("ep", None),
        P("ep", None),
        P("ep", None, "tp"),
        P("ep", None, "tp"),
        P("ep", "tp", None),
    )
    out_specs = P("ep", "tp")
    return jax.shard_map(shards, mesh=mesh, in_specs=in_specs, out_specs=out_specs, check_vma=False)
```

```python
import functools

import jax
import jax.numpy as jnp
from jax import lax
from jax.experimental import pallas as pl
from jax.experimental.pallas import tpu as pltpu
from jax.sharding import PartitionSpec as P

EPS = 1e-06
MIB = 1024 * 1024
VMEM = pl.BlockSpec(memory_space=pltpu.VMEM)
SMEM = pl.BlockSpec(memory_space=pltpu.SMEM)
HBM = pl.BlockSpec(memory_space=pltpu.HBM)


def swap(value, axis, bits):
    n = lax.axis_size(axis)
    return lax.ppermute(value, axis, [(i, i ^ bits) for i in range(n)])


def dispatch_kernel(me_ref, ids_ref, tokens_ref, *outs):
    rows = tokens_ref.shape[0]
    cap = outs[0].shape[0]
    expert = lax.broadcasted_iota(jnp.int32, (len(outs), rows), 0) ^ me_ref[0]
    named = (ids_ref[0:1, :] == expert) | (ids_ref[1:2, :] == expert)
    earlier = lax.broadcasted_iota(jnp.int32, (rows, rows), 0) < lax.broadcasted_iota(jnp.int32, (rows, rows), 1)
    slots = jnp.dot(
        named.astype(jnp.bfloat16), earlier.astype(jnp.bfloat16), preferred_element_type=jnp.float32
    ).astype(jnp.int32)
    slots = jnp.where(named, slots, -1)
    place = lax.broadcasted_iota(jnp.int32, (cap, rows), 0)
    tokens = tokens_ref[...]
    for k, out in enumerate(outs):
        pick = (place == slots[k : k + 1, :]).astype(jnp.float32).astype(jnp.bfloat16)
        out[...] = jnp.dot(pick, tokens, preferred_element_type=jnp.float32).astype(jnp.bfloat16)


def dispatch(me, ids, tokens, n_out, cap):
    return pl.pallas_call(
        dispatch_kernel,
        out_shape=[jax.ShapeDtypeStruct((cap, tokens.shape[1]), jnp.bfloat16)] * n_out,
        in_specs=[SMEM, VMEM, VMEM],
        out_specs=[VMEM] * n_out,
        compiler_params=pltpu.CompilerParams(vmem_limit_bytes=8 * MIB),
        name="dispatch",
    )(me, ids, tokens)


def join_kernel(*refs):
    out, at = refs[-1], 0
    for ref in refs[:-1]:
        out[at : at + ref.shape[0], :] = ref[...]
        at += ref.shape[0]


def join(arrays):
    shape = (sum(a.shape[0] for a in arrays), arrays[0].shape[1])
    return pl.pallas_call(
        join_kernel,
        out_shape=jax.ShapeDtypeStruct(shape, arrays[0].dtype),
        in_specs=[VMEM] * len(arrays),
        out_specs=VMEM,
        compiler_params=pltpu.CompilerParams(vmem_limit_bytes=4 * MIB),
        name="join",
    )(*arrays)


def sum_kernel(*refs, n_in, size, blocks):
    outs = refs[n_in:]
    step = size // len(outs)
    for i, out in enumerate(outs):
        total = 0.0
        for ref, block in zip(refs, blocks):
            total = total + ref[block * size + i * step : block * size + (i + 1) * step, :].astype(jnp.float32)
        out[...] = total.astype(jnp.bfloat16)


def add_up(addends, size, n_out):
    width = addends[0][0].shape[1]
    return pl.pallas_call(
        functools.partial(sum_kernel, n_in=len(addends), size=size, blocks=[b for _, b in addends]),
        out_shape=[jax.ShapeDtypeStruct((size // n_out, width), jnp.bfloat16)] * n_out,
        in_specs=[VMEM] * len(addends),
        out_specs=[VMEM] * n_out,
        compiler_params=pltpu.CompilerParams(vmem_limit_bytes=4 * MIB),
        name="sum",
    )(*[a for a, _ in addends])


def place_kernel(me_ref, ids_ref, share_ref, target_out, share_out, *, experts, cap):
    rows = ids_ref.shape[1]
    expert = lax.broadcasted_iota(jnp.int32, (experts, rows), 0)
    chosen = [ids_ref[j : j + 1, :] == expert ^ me_ref[0] for j in range(2)]
    earlier = lax.broadcasted_iota(jnp.int32, (rows, rows), 0) < lax.broadcasted_iota(jnp.int32, (rows, rows), 1)
    named = chosen[0] | chosen[1]
    slots = jnp.dot(named.astype(jnp.bfloat16), earlier.astype(jnp.bfloat16), preferred_element_type=jnp.float32)
    target = slots + (cap * expert).astype(jnp.float32)
    lines = [jnp.sum(jnp.where(c, target, 0.0), axis=0, keepdims=True) for c in chosen]
    lines = lines + [share_ref[0:1, :], share_ref[1:2, :], jnp.zeros((4, rows), jnp.float32)]
    columns = jnp.transpose(jnp.concatenate(lines, axis=0))
    target_out[...] = columns[:, 0:2].astype(jnp.int32)
    share_out[...] = columns[:, 2:4]


def combine_kernel(target_ref, share_ref, *refs):
    blocks, out, table = refs[:-2], refs[-2], refs[-1]
    cap = blocks[0].shape[0]
    for k, block in enumerate(blocks):
        table[k * cap : (k + 1) * cap, :] = block[...]
    rows = out.shape[0]
    total = jnp.zeros(out.shape, jnp.float32)
    slot = lax.broadcasted_iota(jnp.int32, (rows, table.shape[0]), 1)
    for j in range(2):
        pick = (slot == target_ref[:, j : j + 1]).astype(jnp.float32).astype(jnp.bfloat16)
        found = jnp.dot(pick, table[...], preferred_element_type=jnp.float32)
        total = total + found * share_ref[:, j : j + 1]
    out[...] = total.astype(jnp.bfloat16)


def hold_kernel(*refs):
    copies = [pltpu.make_async_copy(refs[i], refs[3 + i], refs[-1].at[i]) for i in range(3)]
    for copy in copies:
        copy.start()
    for copy in copies:
        copy.wait()


def hold(weights):
    return pl.pallas_call(
        hold_kernel,
        out_shape=[jax.ShapeDtypeStruct(w.shape, w.dtype) for w in weights],
        in_specs=[HBM] * 3,
        out_specs=[VMEM] * 3,
        scratch_shapes=[pltpu.SemaphoreType.DMA((3,))],
        compiler_params=pltpu.CompilerParams(vmem_limit_bytes=38 * MIB),
        name="hold",
    )(*weights)


def ffn_kernel(me_ref, *refs, n_tp, rows, block):
    pieces, heads = refs[:n_tp], refs[n_tp : 2 * n_tp]
    gate_ref, up_ref, down_ref, keep_ref, give_ref, normed_ref, hidden_ref = refs[2 * n_tp :]
    me = me_ref[0]
    width = pieces[0].shape[1]
    squares = jnp.zeros((rows, 1), jnp.float32)
    for piece in pieces:
        values = piece[:rows, :].astype(jnp.float32)
        squares = squares + jnp.sum(values * values, axis=1, keepdims=True)
    factor = lax.rsqrt(squares / gate_ref.shape[0] + EPS)
    for j, (piece, head) in enumerate(zip(pieces, heads)):
        at = pl.ds(pl.multiple_of((me ^ j) * width, width), width)
        gain = head[rows : rows + 16, :].astype(jnp.float32)[0:1, :]
        normed_ref[:, at] = (piece[:rows, :].astype(jnp.float32) * factor * gain).astype(jnp.bfloat16)
    normed = normed_ref[...]
    for o in range(0, gate_ref.shape[1], block):
        gate = jnp.dot(normed, gate_ref[:, o : o + block], preferred_element_type=jnp.float32)
        upper = jnp.dot(normed, up_ref[:, o : o + block], preferred_element_type=jnp.float32)
        hidden_ref[:, o : o + block] = (gate / (1.0 + jnp.exp(-gate)) * upper).astype(jnp.bfloat16)
    hidden = hidden_ref[...]
    for j in range(n_tp):
        at = pl.ds(pl.multiple_of((me ^ j) * width, width), width)
        term = jnp.dot(hidden, down_ref[:, at], preferred_element_type=jnp.float32).astype(jnp.bfloat16)
        ref = (keep_ref, give_ref)[j & 1]
        ref[(j >> 1) * rows : ((j >> 1) + 1) * rows, :] = term


def ffn(me, rows, pieces, heads, weights):
    n_tp, width = len(pieces), pieces[0].shape[1]
    d, f = weights[0].shape
    half = jax.ShapeDtypeStruct((n_tp // 2 * rows, width), jnp.bfloat16)
    return pl.pallas_call(
        functools.partial(ffn_kernel, n_tp=n_tp, rows=rows, block=min(f, 512)),
        out_shape=[half, half],
        in_specs=[SMEM] + [VMEM] * (2 * n_tp + 3),
        out_specs=[VMEM] * 2,
        scratch_shapes=[pltpu.VMEM((rows, d), jnp.bfloat16), pltpu.VMEM((rows, f), jnp.bfloat16)],
        compiler_params=pltpu.CompilerParams(vmem_limit_bytes=10 * MIB),
        cost_estimate=pl.CostEstimate(flops=6 * rows * d * f, transcendentals=rows * f, bytes_accessed=6 * d * f),
        name="ffn",
    )(me, *pieces, *heads, *weights)


def shards(tokens, norm_gain, expert_ids, gate_share, gate_weight, up_weight, down_weight):
    n_ep, n_tp = lax.axis_size("ep"), lax.axis_size("tp")
    rows, width = tokens.shape
    experts = n_ep
    cap = 4 * rows // experts
    ep = lax.axis_index("ep").reshape(1).astype(jnp.int32)
    tp = lax.axis_index("tp").reshape(1).astype(jnp.int32)
    ep, tp = lax.optimization_barrier((ep, tp))
    bits = [1 << b for b in range(n_tp.bit_length() - 1)]
    bits.reverse()

    ids = expert_ids.T
    near = dispatch(ep, ids, tokens, n_ep, cap)
    arrived = [near[0]] + [swap(near[k], "ep", k) for k in range(1, n_ep)]

    weights = hold([gate_weight[0], up_weight[0], down_weight[0]])
    gain = jnp.broadcast_to(norm_gain.reshape(1, width), (16, width))

    place = pl.pallas_call(
        functools.partial(place_kernel, experts=experts, cap=cap),
        out_shape=(jax.ShapeDtypeStruct((rows, 2), jnp.int32), jax.ShapeDtypeStruct((rows, 2), jnp.float32)),
        in_specs=[SMEM, VMEM, VMEM],
        out_specs=(VMEM, VMEM),
        compiler_params=pltpu.CompilerParams(vmem_limit_bytes=8 * MIB),
        name="place",
    )
    target, share = place(ep, ids, gate_share.T)

    group = n_ep // 4
    back = [None] * n_ep
    for c in range(4):
        names = list(range(c * group, (c + 1) * group))
        pieces = {0: join([arrived[k] for k in names] + [gain] * (c == 0))}
        for bit in bits:
            pieces.update({o ^ bit: swap(p, "tp", bit) for o, p in pieces.items()})
        pieces = [pieces[o] for o in range(n_tp)]
        heads = heads if c else pieces
        keep, give = ffn(tp, group * cap, pieces, heads, weights)
        got = swap(give, "tp", 1)
        size = group * cap
        parts = [[(keep, i), (got, i)] for i in range(n_tp // 2)]
        while len(parts) > 1:
            bit = n_tp // len(parts)
            sent = [swap(add_up(p, size, 1)[0], "tp", bit) for p in parts[1::2]]
            parts = [p + [(s, 0)] for p, s in zip(parts[0::2], sent)]
        for k, piece in zip(names, add_up(parts[0], size, group)):
            back[k] = swap(piece, "ep", k) if k else piece

    return pl.pallas_call(
        combine_kernel,
        out_shape=jax.ShapeDtypeStruct((rows, width), jnp.bfloat16),
        in_specs=[VMEM] * (2 + n_ep),
        out_specs=VMEM,
        scratch_shapes=[pltpu.VMEM((experts * cap, width), jnp.bfloat16)],
        compiler_params=pltpu.CompilerParams(vmem_limit_bytes=8 * MIB),
        name="combine",
    )(target, share, *back)


def solution(mesh):
    in_specs = (
        P("ep", "tp"),
        P("tp"),
        P("ep", None),
        P("ep", None),
        P("ep", None, "tp"),
        P("ep", None, "tp"),
        P("ep", "tp", None),
    )
    out_specs = P("ep", "tp")

    return jax.shard_map(shards, mesh=mesh, in_specs=in_specs, out_specs=out_specs, check_vma=False)
```

```python
import functools

import jax
import jax.numpy as jnp
from jax import lax
from jax.experimental import pallas as pl
from jax.experimental.pallas import tpu as pltpu
from jax.sharding import PartitionSpec as P

EPS = 1e-06
MIB = 1024 * 1024
VMEM = pl.BlockSpec(memory_space=pltpu.VMEM)
SMEM = pl.BlockSpec(memory_space=pltpu.SMEM)
HBM = pl.BlockSpec(memory_space=pltpu.HBM)


def swap(value, axis, bits):
    n = lax.axis_size(axis)
    return lax.ppermute(value, axis, [(i, i ^ bits) for i in range(n)])


def dispatch_kernel(me_ref, ids_ref, tokens_ref, *outs):
    rows = tokens_ref.shape[0]
    cap = outs[0].shape[0]
    expert = lax.broadcasted_iota(jnp.int32, (len(outs), rows), 0) ^ me_ref[0]
    named = (ids_ref[0:1, :] == expert) | (ids_ref[1:2, :] == expert)
    earlier = lax.broadcasted_iota(jnp.int32, (rows, rows), 0) < lax.broadcasted_iota(jnp.int32, (rows, rows), 1)
    slots = jnp.dot(
        named.astype(jnp.bfloat16), earlier.astype(jnp.bfloat16), preferred_element_type=jnp.float32
    ).astype(jnp.int32)
    slots = jnp.where(named, slots, -1)
    place = lax.broadcasted_iota(jnp.int32, (cap, rows), 0)
    tokens = tokens_ref[...]
    for k, out in enumerate(outs):
        pick = (place == slots[k : k + 1, :]).astype(jnp.float32).astype(jnp.bfloat16)
        out[...] = jnp.dot(pick, tokens, preferred_element_type=jnp.float32).astype(jnp.bfloat16)


def dispatch(me, ids, tokens, n_out, cap):
    return pl.pallas_call(
        dispatch_kernel,
        out_shape=[jax.ShapeDtypeStruct((cap, tokens.shape[1]), jnp.bfloat16)] * n_out,
        in_specs=[SMEM, VMEM, VMEM],
        out_specs=[VMEM] * n_out,
        compiler_params=pltpu.CompilerParams(vmem_limit_bytes=8 * MIB),
        name="dispatch",
    )(me, ids, tokens)


def join_kernel(*refs):
    out, at = refs[-1], 0
    for ref in refs[:-1]:
        out[at : at + ref.shape[0], :] = ref[...]
        at += ref.shape[0]


def join(arrays):
    shape = (sum(a.shape[0] for a in arrays), arrays[0].shape[1])
    return pl.pallas_call(
        join_kernel,
        out_shape=jax.ShapeDtypeStruct(shape, arrays[0].dtype),
        in_specs=[VMEM] * len(arrays),
        out_specs=VMEM,
        compiler_params=pltpu.CompilerParams(vmem_limit_bytes=4 * MIB),
        name="join",
    )(*arrays)


def sum_kernel(*refs, n_in, size, blocks):
    outs = refs[n_in:]
    step = size // len(outs)
    for i, out in enumerate(outs):
        total = 0.0
        for ref, block in zip(refs, blocks):
            total = total + ref[block * size + i * step : block * size + (i + 1) * step, :].astype(jnp.float32)
        out[...] = total.astype(jnp.bfloat16)


def add_up(addends, size, n_out):
    width = addends[0][0].shape[1]
    return pl.pallas_call(
        functools.partial(sum_kernel, n_in=len(addends), size=size, blocks=[b for _, b in addends]),
        out_shape=[jax.ShapeDtypeStruct((size // n_out, width), jnp.bfloat16)] * n_out,
        in_specs=[VMEM] * len(addends),
        out_specs=[VMEM] * n_out,
        compiler_params=pltpu.CompilerParams(vmem_limit_bytes=4 * MIB),
        name="sum",
    )(*[a for a, _ in addends])


def place_kernel(me_ref, ids_ref, share_ref, target_out, share_out, *, experts, cap):
    rows = ids_ref.shape[1]
    expert = lax.broadcasted_iota(jnp.int32, (experts, rows), 0)
    chosen = [ids_ref[j : j + 1, :] == expert ^ me_ref[0] for j in range(2)]
    earlier = lax.broadcasted_iota(jnp.int32, (rows, rows), 0) < lax.broadcasted_iota(jnp.int32, (rows, rows), 1)
    named = chosen[0] | chosen[1]
    slots = jnp.dot(named.astype(jnp.bfloat16), earlier.astype(jnp.bfloat16), preferred_element_type=jnp.float32)
    target = slots + (cap * expert).astype(jnp.float32)
    lines = [jnp.sum(jnp.where(c, target, 0.0), axis=0, keepdims=True) for c in chosen]
    lines = lines + [share_ref[0:1, :], share_ref[1:2, :], jnp.zeros((4, rows), jnp.float32)]
    columns = jnp.transpose(jnp.concatenate(lines, axis=0))
    target_out[...] = columns[:, 0:2].astype(jnp.int32)
    share_out[...] = columns[:, 2:4]


def combine_kernel(target_ref, share_ref, *refs, first, n_blocks):
    blocks, before, out, table = refs[:n_blocks], refs[n_blocks:-2], refs[-2], refs[-1]
    cap = blocks[0].shape[0]
    for k, block in enumerate(blocks):
        table[k * cap : (k + 1) * cap, :] = block[...]
    slot = lax.broadcasted_iota(jnp.int32, (out.shape[0], table.shape[0]), 1) + first * cap
    total = before[0][...] if before else jnp.zeros(out.shape, jnp.float32)
    for j in range(2):
        pick = (slot == target_ref[:, j : j + 1]).astype(jnp.float32).astype(jnp.bfloat16)
        found = jnp.dot(pick, table[...], preferred_element_type=jnp.float32)
        total = total + found * share_ref[:, j : j + 1]
    out[...] = total.astype(out.dtype)


def combine(target, share, first, blocks, before, dtype):
    cap, width = blocks[0].shape
    return pl.pallas_call(
        functools.partial(combine_kernel, first=first, n_blocks=len(blocks)),
        out_shape=jax.ShapeDtypeStruct((target.shape[0], width), dtype),
        in_specs=[VMEM] * (2 + len(blocks) + len(before)),
        out_specs=VMEM,
        scratch_shapes=[pltpu.VMEM((len(blocks) * cap, width), jnp.bfloat16)],
        compiler_params=pltpu.CompilerParams(vmem_limit_bytes=8 * MIB),
        name="combine",
    )(target, share, *blocks, *before)


def hold_kernel(*refs):
    copies = [pltpu.make_async_copy(refs[i], refs[3 + i], refs[-1].at[i]) for i in range(3)]
    for copy in copies:
        copy.start()
    for copy in copies:
        copy.wait()


def hold(weights):
    return pl.pallas_call(
        hold_kernel,
        out_shape=[jax.ShapeDtypeStruct(w.shape, w.dtype) for w in weights],
        in_specs=[HBM] * 3,
        out_specs=[VMEM] * 3,
        scratch_shapes=[pltpu.SemaphoreType.DMA((3,))],
        compiler_params=pltpu.CompilerParams(vmem_limit_bytes=38 * MIB),
        name="hold",
    )(*weights)


def ffn_kernel(me_ref, *refs, n_tp, rows, block):
    pieces, heads = refs[:n_tp], refs[n_tp : 2 * n_tp]
    gate_ref, up_ref, down_ref, keep_ref, give_ref, normed_ref, hidden_ref = refs[2 * n_tp :]
    me = me_ref[0]
    width = pieces[0].shape[1]
    squares = jnp.zeros((rows, 1), jnp.float32)
    for piece in pieces:
        values = piece[:rows, :].astype(jnp.float32)
        squares = squares + jnp.sum(values * values, axis=1, keepdims=True)
    factor = lax.rsqrt(squares / gate_ref.shape[0] + EPS)
    for j, (piece, head) in enumerate(zip(pieces, heads)):
        at = pl.ds(pl.multiple_of((me ^ j) * width, width), width)
        gain = head[rows : rows + 16, :].astype(jnp.float32)[0:1, :]
        normed_ref[:, at] = (piece[:rows, :].astype(jnp.float32) * factor * gain).astype(jnp.bfloat16)
    normed = normed_ref[...]
    for o in range(0, gate_ref.shape[1], block):
        gate = jnp.dot(normed, gate_ref[:, o : o + block], preferred_element_type=jnp.float32)
        upper = jnp.dot(normed, up_ref[:, o : o + block], preferred_element_type=jnp.float32)
        hidden_ref[:, o : o + block] = (gate / (1.0 + jnp.exp(-gate)) * upper).astype(jnp.bfloat16)
    hidden = hidden_ref[...]
    for j in range(n_tp):
        at = pl.ds(pl.multiple_of((me ^ j) * width, width), width)
        term = jnp.dot(hidden, down_ref[:, at], preferred_element_type=jnp.float32).astype(jnp.bfloat16)
        ref = (keep_ref, give_ref)[j & 1]
        ref[(j >> 1) * rows : ((j >> 1) + 1) * rows, :] = term


def ffn(me, rows, pieces, heads, weights):
    n_tp, width = len(pieces), pieces[0].shape[1]
    d, f = weights[0].shape
    half = jax.ShapeDtypeStruct((n_tp // 2 * rows, width), jnp.bfloat16)
    return pl.pallas_call(
        functools.partial(ffn_kernel, n_tp=n_tp, rows=rows, block=min(f, 512)),
        out_shape=[half, half],
        in_specs=[SMEM] + [VMEM] * (2 * n_tp + 3),
        out_specs=[VMEM] * 2,
        scratch_shapes=[pltpu.VMEM((rows, d), jnp.bfloat16), pltpu.VMEM((rows, f), jnp.bfloat16)],
        compiler_params=pltpu.CompilerParams(vmem_limit_bytes=10 * MIB),
        cost_estimate=pl.CostEstimate(flops=6 * rows * d * f, transcendentals=rows * f, bytes_accessed=6 * d * f),
        name="ffn",
    )(me, *pieces, *heads, *weights)


def shards(tokens, norm_gain, expert_ids, gate_share, gate_weight, up_weight, down_weight):
    n_ep, n_tp = lax.axis_size("ep"), lax.axis_size("tp")
    rows, width = tokens.shape
    experts = n_ep
    cap = 4 * rows // experts
    ep = lax.axis_index("ep").reshape(1).astype(jnp.int32)
    tp = lax.axis_index("tp").reshape(1).astype(jnp.int32)
    ep, tp = lax.optimization_barrier((ep, tp))
    bits = [1 << b for b in range(n_tp.bit_length() - 1)]
    bits.reverse()

    ids = expert_ids.T
    near = dispatch(ep, ids, tokens, n_ep, cap)
    arrived = [near[0]] + [swap(near[k], "ep", k) for k in range(1, n_ep)]

    weights = hold([gate_weight[0], up_weight[0], down_weight[0]])
    gain = jnp.broadcast_to(norm_gain.reshape(1, width), (16, width))

    place = pl.pallas_call(
        functools.partial(place_kernel, experts=experts, cap=cap),
        out_shape=(jax.ShapeDtypeStruct((rows, 2), jnp.int32), jax.ShapeDtypeStruct((rows, 2), jnp.float32)),
        in_specs=[SMEM, VMEM, VMEM],
        out_specs=(VMEM, VMEM),
        compiler_params=pltpu.CompilerParams(vmem_limit_bytes=8 * MIB),
        name="place",
    )
    target, share = place(ep, ids, gate_share.T)

    group = n_ep // 4
    back = [None] * n_ep
    for c in range(4):
        names = list(range(c * group, (c + 1) * group))
        pieces = {0: join([arrived[k] for k in names] + [gain] * (c == 0))}
        for bit in bits:
            pieces.update({o ^ bit: swap(p, "tp", bit) for o, p in pieces.items()})
        pieces = [pieces[o] for o in range(n_tp)]
        heads = heads if c else pieces
        keep, give = ffn(tp, group * cap, pieces, heads, weights)
        got = swap(give, "tp", 1)
        size = group * cap
        parts = [[(keep, i), (got, i)] for i in range(n_tp // 2)]
        while len(parts) > 1:
            bit = n_tp // len(parts)
            sent = [swap(add_up(p, size, 1)[0], "tp", bit) for p in parts[1::2]]
            parts = [p + [(s, 0)] for p, s in zip(parts[0::2], sent)]
        for k, piece in zip(names, add_up(parts[0], size, group)):
            back[k] = swap(piece, "ep", k) if k else piece

    most = combine(target, share, group, back[group:], [], jnp.float32)
    return combine(target, share, 0, back[:group], [most], jnp.bfloat16)


def solution(mesh):
    in_specs = (
        P("ep", "tp"),
        P("tp"),
        P("ep", None),
        P("ep", None),
        P("ep", None, "tp"),
        P("ep", None, "tp"),
        P("ep", "tp", None),
    )
    out_specs = P("ep", "tp")

    return jax.shard_map(shards, mesh=mesh, in_specs=in_specs, out_specs=out_specs, check_vma=False)
```
